32 devices in a mesh: grp: 2 (over y), kv: 4 (over z), tp: 4 (over x, core).
Axes of the slice: x: 2, y: 2, z: 4, core: 2. Of those that a mesh axis runs over, the one named last changes fastest.
Arguments:
- tokens: bfloat16 [32, 4096], P('grp', ('kv', 'tp')), parts along dimension 0, may hold values from -50 to 50
- mix_gain: bfloat16 [4096], P('kv'), may hold values from 0.099609375 to 1.8984375
- w_query: bfloat16 [4096, 2048], P('kv', 'tp'), may hold values from -0.09375 to 0.09375
- w_forget: bfloat16 [4096, 2048], P('kv', 'tp'), may hold values from -0.09375 to 0.09375
- w_input: bfloat16 [4096, 2048], P('kv', 'tp'), may hold values from -0.09375 to 0.09375
- w_outgate: bfloat16 [4096, 2048], P('kv', 'tp'), may hold values from -0.09375 to 0.09375
- lower_bound: float32 [2048], P('tp'), may hold values from 0.05 to 0.9
- state: float32 [32, 16, 128, 128], P(('grp', 'kv'), 'tp'), parts along dimension 0, may hold values from -4 to 4
- head_gain: bfloat16 [128], replicated, may hold values from 0.099609375 to 1.8984375
- w_mixout: bfloat16 [2048, 4096], P('tp', 'kv'), may hold values from -0.125 to 0.125
- ffn_gain: bfloat16 [4096], P('kv'), may hold values from 0.099609375 to 1.8984375
- w_gate: bfloat16 [4096, 11264], P('kv', 'tp'), may hold values from -0.09375 to 0.09375
- w_up: bfloat16 [4096, 11264], P('kv', 'tp'), may hold values from -0.09375 to 0.09375
- w_down: bfloat16 [11264, 4096], P('tp', 'kv'), may hold values from -0.0546875 to 0.0546875
Outputs:
- mixed: bfloat16 [32, 4096], P('grp', ('kv', 'tp')), parts along dimension 0
- new_state: float32 [32, 16, 128, 128], P(('grp', 'kv'), 'tp'), parts along dimension 0
The draws below stay inside these ranges and needn't reach their ends.
There are 2 independent parts, one for each index of `grp`. The reference program is written for one: setup_inputs(seed, part) draws one part's arguments, and reference() takes and returns one part's arrays. A program takes and returns all parts, laid end to end along the dimension named above; an argument that names none is the same for every part. Nothing has to cross between parts.
All inputs are finite; a program needn't handle non-finite values.
Results may differ from the reference program's by a relative error of at most 0.01.
Values may be sent and summed in bfloat16 or wider, within the bound.
A program may use at most 64 MiB of HBM per device.

```python
import jax
import jax.numpy as jnp
from jax import lax

D = 4096
HEADS = 16
HEAD_DIM = 128
FF = 11264
BATCH = 16
KEY_WIDTH = 2048


def draw_tokens(key, part):
    key_base = jax.random.fold_in(key, 11)
    key_cols = jax.random.fold_in(key, 12)
    block_scale = jnp.exp(jax.random.uniform(key_cols, (D // 16,), jnp.float32, -1.1, 1.1))
    column_scale = jnp.repeat(block_scale, 16)[None, :]
    base = jnp.clip(jax.random.normal(key_base, (BATCH, D), jnp.float32), -4.0, 4.0)
    return (base * column_scale).astype(jnp.bfloat16)


def shard_levels(rng, shape, cuts, low, largest):
    def one(position, blocks):
        draws = jax.random.uniform(jax.random.fold_in(jax.random.fold_in(rng, 6), position), (blocks,), jnp.float32, low / len(cuts), largest / len(cuts))
        return jnp.repeat(jnp.exp(draws), shape[position] // blocks).reshape((-1,) + (1,) * (len(shape) - position - 1))

    loudness = one(*cuts[0])
    for cut in cuts[1:]:
        loudness = loudness * one(*cut)
    return loudness


def noise(key, dims, width, most, pieces=(), kind=jnp.bfloat16):
    entries = jax.random.normal(key, dims, jnp.float32) * width
    if len(pieces) > 0:
        entries = shard_levels(key, dims, pieces, -0.22, 0.18) * entries
    return jnp.clip(entries, min=-most, max=most).astype(kind)


def setup_inputs(seed: int = 0, part: int = 0) -> dict:
    arg_keys = jax.random.split(jax.random.key(seed), 15)
    part_splits = jax.random.split(jax.random.fold_in(arg_keys[14], part), 15)
    return {
        "tokens": draw_tokens(jax.random.fold_in(jax.random.fold_in(arg_keys[14], part), 71), part),
        "mix_gain": jnp.clip(1.0 + 0.18 * jax.random.normal(arg_keys[1], (D,), jnp.float32), 0.099609375, 1.8984375).astype(jnp.bfloat16),
        "w_query": noise(arg_keys[2], (D, KEY_WIDTH), D ** -0.5, 0.09375, ((0, 4), (1, 4))),
        "w_forget": noise(arg_keys[3], (D, KEY_WIDTH), D ** -0.5, 0.09375, ((0, 4), (1, 4))),
        "w_input": noise(arg_keys[4], (D, KEY_WIDTH), D ** -0.5, 0.09375, ((0, 4), (1, 4))),
        "w_outgate": noise(arg_keys[5], (D, KEY_WIDTH), D ** -0.5, 0.09375, ((0, 4), (1, 4))),
        "lower_bound": jnp.clip(0.05 + 0.84999998 * jax.random.uniform(arg_keys[6], (KEY_WIDTH,), jnp.float32) ** shard_levels(arg_keys[6], (KEY_WIDTH,), ((0, 4),), -0.2, 0.2), 0.05, 0.9),
        "state": noise(part_splits[7], (BATCH, HEADS, HEAD_DIM, HEAD_DIM), 0.5, 4.0, ((0, 4), (1, 4)), jnp.float32),
        "head_gain": jnp.clip(1.0 + 0.18 * jax.random.normal(arg_keys[8], (HEAD_DIM,), jnp.float32), 0.099609375, 1.8984375).astype(jnp.bfloat16),
        "w_mixout": noise(arg_keys[9], (KEY_WIDTH, D), KEY_WIDTH ** -0.5, 0.125, ((0, 4), (1, 4))),
        "ffn_gain": jnp.clip(1.0 + 0.18 * jax.random.normal(arg_keys[10], (D,), jnp.float32), 0.099609375, 1.8984375).astype(jnp.bfloat16),
        "w_gate": noise(arg_keys[11], (D, FF), D ** -0.5, 0.09375, ((0, 4), (1, 4))),
        "w_up": noise(arg_keys[12], (D, FF), D ** -0.5, 0.09375, ((0, 4), (1, 4))),
        "w_down": noise(arg_keys[13], (FF, D), FF ** -0.5, 0.0546875, ((0, 4), (1, 4))),
    }


eps = 0.1

def reference(tokens, mix_gain, w_query, w_forget, w_input, w_outgate, lower_bound, state, head_gain, w_mixout, ffn_gain, w_gate, w_up, w_down):
    batch = tokens.shape[0]
    tokens_f = tokens.astype(jnp.float32)
    normed = (tokens_f * mix_gain.astype(jnp.float32)).astype(jnp.bfloat16)
    inv_rms = lax.rsqrt(lax.optimization_barrier(jnp.mean(tokens_f * tokens_f, axis=1, keepdims=True)) + eps)

    def heads_of(weight):
        product = jnp.dot(normed, weight, preferred_element_type=jnp.float32) * inv_rms
        return product.reshape(batch, HEADS, HEAD_DIM)
    query_act = jax.nn.silu(heads_of(w_query))
    forget_raw = heads_of(w_forget)
    values_in = heads_of(w_input)
    gate_raw = heads_of(w_outgate)
    bounds = lower_bound.reshape(HEADS, HEAD_DIM)
    forget = bounds + (1.0 - bounds) * jax.nn.sigmoid(forget_raw)
    key_in = (1.0 - bounds) * jax.nn.sigmoid(-forget_raw)
    new_state = forget[..., None] * state + key_in[..., None] * values_in[:, :, None, :]
    readout = lax.optimization_barrier(jnp.sum(query_act[..., None] * new_state, axis=2))
    head_rms = lax.rsqrt(lax.optimization_barrier(jnp.mean(readout * readout, axis=-1, keepdims=True)) + eps)
    gated_out = readout * head_rms * head_gain.astype(jnp.float32) * jax.nn.silu(gate_raw)
    gated_out = gated_out.reshape(batch, HEADS * HEAD_DIM).astype(jnp.bfloat16)
    mix_sum = jnp.dot(gated_out, w_mixout, preferred_element_type=jnp.float32)
    resid = (tokens_f + mix_sum).astype(jnp.bfloat16)
    resid_f = resid.astype(jnp.float32)
    normed_ffn = (resid_f * ffn_gain.astype(jnp.float32)).astype(jnp.bfloat16)
    inv_rms_ffn = lax.rsqrt(lax.optimization_barrier(jnp.mean(resid_f * resid_f, axis=1, keepdims=True)) + eps)
    gate_sum = jnp.dot(normed_ffn, w_gate, preferred_element_type=jnp.float32) * inv_rms_ffn
    up_sum = jnp.dot(normed_ffn, w_up, preferred_element_type=jnp.float32) * inv_rms_ffn
    hidden = (jax.nn.silu(gate_sum) * up_sum).astype(jnp.bfloat16)
    down_sum = jnp.dot(hidden, w_down, preferred_element_type=jnp.float32)
    mixed = (resid_f + down_sum).astype(jnp.bfloat16)
    return (mixed, new_state)
```

```python
import functools

import jax
import jax.numpy as jnp
from jax import lax
from jax.experimental import pallas as pl
from jax.experimental.pallas import tpu as pltpu
from jax.sharding import PartitionSpec as P

eps = 0.1
LANES = 128
F32 = jnp.float32
BF16 = jnp.bfloat16


def split_squares(squares):
    wide = jnp.broadcast_to(squares, (squares.shape[0], LANES))
    high = wide.astype(BF16).astype(F32)
    lane = lax.broadcasted_iota(jnp.int32, wide.shape, 1)
    return jnp.where(lane < LANES // 2, high, wide - high)


def join_squares(tile):
    return tile[:, :1] + tile[:, LANES // 2 : LANES // 2 + 1]


def kernel(
    n_kv,
    n_tp,
    tokens,
    mix_gain,
    w_query,
    w_forget,
    w_input,
    w_outgate,
    lower_bound,
    state,
    head_gain,
    w_mixout,
    ffn_gain,
    w_gate,
    w_up,
    w_down,
    mixed,
    new_state,
    proj_v,
    state_v,
    mixout_v,
    gate_v,
    up_v,
    down_v,
    next_v,
    tok_buf,
    proj_f,
    proj_send,
    proj_recv,
    read_buf,
    read_f,
    mix_buf,
    resid_buf,
    ffn_f,
    ffn_send,
    ffn_recv,
    hid_buf,
    hid_f,
    down_send,
    down_recv,
    load_sem,
    tok_s,
    tok_r,
    proj_s,
    proj_r,
    read_s,
    read_r,
    mix_s,
    mix_r,
    ffn_s,
    ffn_r,
    hid_s,
    hid_r,
    down_s,
    down_r,
):
    kv = lax.axis_index("kv")
    tp = lax.axis_index("tp")
    rows, heads, size, _ = state.shape
    width = w_query.shape[1]
    hidden = w_gate.shape[1]
    cols = tokens.shape[1]
    model = w_query.shape[0] * n_kv

    loads = [
        pltpu.make_async_copy(src, dst, load_sem.at[i])
        for i, (src, dst) in enumerate(
            [
                (tokens, tok_buf.at[tp]),
                (w_query, proj_v.at[0]),
                (w_forget, proj_v.at[1]),
                (w_input, proj_v.at[2]),
                (w_outgate, proj_v.at[3]),
                (state, state_v),
                (w_mixout, mixout_v),
                (w_gate, gate_v),
                (w_up, up_v),
                (w_down, down_v),
            ]
        )
    ]
    for load in loads:
        load.start()

    barrier = pltpu.get_barrier_semaphore()
    for d in range(1, n_tp):
        pl.semaphore_signal(barrier, inc=1, device_id={"tp": lax.rem(tp + d, n_tp)})
    for d in range(1, n_kv):
        pl.semaphore_signal(barrier, inc=1, device_id={"kv": lax.rem(kv + d, n_kv)})
    pl.semaphore_wait(barrier, n_tp - 1 + n_kv - 1)

    sent = []

    def exchange(axis, me, n, source, target, send_sem, recv_sem):
        copies = []
        for d in reversed(range(1, n)):
            peer = lax.rem(me + d, n)
            copy = pltpu.make_async_remote_copy(
                src_ref=source(peer),
                dst_ref=target(d),
                send_sem=send_sem.at[d - 1],
                recv_sem=recv_sem.at[d - 1],
                device_id={axis: peer},
            )
            copy.start()
            copies.append(copy)
        sent.extend(copies)
        return copies

    loads[0].wait()
    own = tok_buf.at[tp]
    for copy in exchange("tp", tp, n_tp, lambda p: own, lambda d: own, tok_s, tok_r):
        copy.wait_recv()
    block = jnp.concatenate([tok_buf[i].astype(F32) for i in range(n_tp)], axis=1)
    normed = (block * mix_gain[...].astype(F32)).astype(BF16)
    proj_f[:, 4 * width :] = split_squares(jnp.sum(block * block, axis=1, keepdims=True))

    for i in range(4):
        loads[1 + i].wait()
        proj_f[:, i * width : (i + 1) * width] = jnp.dot(
            normed, proj_v[i], preferred_element_type=F32
        )
    for j in range(n_kv):
        proj_send[j] = proj_f[j * rows : (j + 1) * rows, :].astype(BF16)
    copies = exchange(
        "kv", kv, n_kv, lambda p: proj_send.at[p], lambda d: proj_recv.at[d - 1], proj_s, proj_r
    )
    total = proj_send[kv].astype(F32)
    loads[5].wait()
    for d, copy in zip(reversed(range(1, n_kv)), copies):
        copy.wait_recv()
        total += proj_recv[d - 1].astype(F32)

    inv_rms = lax.rsqrt(join_squares(total[:, 4 * width :]) / model + eps)
    query_raw, forget_raw, input_raw, gate_raw = (
        total[:, i * width : (i + 1) * width] * inv_rms for i in range(4)
    )
    bounds = lower_bound[...]
    forget = bounds + (1.0 - bounds) * jax.nn.sigmoid(forget_raw)
    key_in = (1.0 - bounds) * jax.nn.sigmoid(-forget_raw)
    query_act = query_raw * jax.nn.sigmoid(query_raw)
    gate_act = gate_raw * jax.nn.sigmoid(gate_raw)
    gain = head_gain[...].astype(F32)
    pad = jnp.zeros((-(3 * rows) % 8, width), F32)
    turned = jnp.concatenate([forget, key_in, query_act, pad], axis=0).T
    pieces = []
    for h in range(heads):
        here = slice(h * size, (h + 1) * size)
        readouts = []
        for b in range(rows):
            forget_c = turned[here, b : b + 1]
            key_c = turned[here, rows + b : rows + b + 1]
            query_c = turned[here, 2 * rows + b : 2 * rows + b + 1]
            after = forget_c * state_v[b, h] + key_c * input_raw[b : b + 1, here]
            next_v[b, h] = after
            readouts.append(jnp.sum(query_c * after, axis=0, keepdims=True))
        readout = jnp.concatenate(readouts, axis=0)
        head_rms = lax.rsqrt(jnp.mean(readout * readout, axis=1, keepdims=True) + eps)
        pieces.append(readout * head_rms * gain * gate_act[:, here])
    read_buf[kv] = jnp.concatenate(pieces, axis=1).astype(BF16)
    own_read = read_buf.at[kv]
    copies = exchange("kv", kv, n_kv, lambda p: own_read, lambda d: own_read, read_s, read_r)
    store = pltpu.make_async_copy(next_v, new_state, load_sem.at[len(loads)])
    store.start()
    loads[6].wait()
    for copy in copies:
        copy.wait_recv()
    for j in range(n_kv):
        read_f[j * rows : (j + 1) * rows, :] = read_buf[j].astype(F32)

    mix_buf[tp] = jnp.dot(
        read_f[...].astype(BF16), mixout_v[...], preferred_element_type=F32
    ).astype(BF16)
    own_mix = mix_buf.at[tp]
    copies = exchange("tp", tp, n_tp, lambda p: own_mix, lambda d: own_mix, mix_s, mix_r)
    for copy in copies:
        copy.wait_recv()
    mix_sum = mix_buf[0].astype(F32)
    for i in range(1, n_tp):
        mix_sum += mix_buf[i].astype(F32)
    resid = (block + mix_sum).astype(BF16).astype(F32)
    for i in range(n_tp):
        resid_buf[i] = resid[:, i * cols : (i + 1) * cols]
    normed_ffn = (resid * ffn_gain[...].astype(F32)).astype(BF16)
    ffn_f[:, 2 * hidden :] = split_squares(jnp.sum(resid * resid, axis=1, keepdims=True))

    loads[7].wait()
    ffn_f[:, :hidden] = jnp.dot(normed_ffn, gate_v[...], preferred_element_type=F32)
    loads[8].wait()
    ffn_f[:, hidden : 2 * hidden] = jnp.dot(normed_ffn, up_v[...], preferred_element_type=F32)
    for j in range(n_kv):
        ffn_send[j] = ffn_f[j * rows : (j + 1) * rows, :].astype(BF16)
    copies = exchange(
        "kv", kv, n_kv, lambda p: ffn_send.at[p], lambda d: ffn_recv.at[d - 1], ffn_s, ffn_r
    )
    total = ffn_send[kv].astype(F32)
    for d, copy in zip(reversed(range(1, n_kv)), copies):
        copy.wait_recv()
        total += ffn_recv[d - 1].astype(F32)
    inv_rms = lax.rsqrt(join_squares(total[:, 2 * hidden :]) / model + eps)
    gate_sum = total[:, :hidden] * inv_rms
    up_sum = total[:, hidden : 2 * hidden] * inv_rms
    hid_buf[kv] = (gate_sum * jax.nn.sigmoid(gate_sum) * up_sum).astype(BF16)
    own_hid = hid_buf.at[kv]
    copies = exchange("kv", kv, n_kv, lambda p: own_hid, lambda d: own_hid, hid_s, hid_r)
    loads[9].wait()
    for copy in copies:
        copy.wait_recv()
    for j in range(n_kv):
        hid_f[j * rows : (j + 1) * rows, :] = hid_buf[j].astype(F32)

    down = jnp.dot(hid_f[...].astype(BF16), down_v[...], preferred_element_type=F32)
    for i in range(n_tp):
        down_send[i] = down[:, i * cols : (i + 1) * cols].astype(BF16)
    copies = exchange(
        "tp", tp, n_tp, lambda p: down_send.at[p], lambda d: down_recv.at[d - 1], down_s, down_r
    )
    result = down_send[tp].astype(F32)
    for d, copy in zip(reversed(range(1, n_tp)), copies):
        copy.wait_recv()
        result += down_recv[d - 1].astype(F32)
    mixed[...] = (resid_buf[tp] + result).astype(BF16)

    for copy in sent:
        copy.wait_send()
    store.wait()


def body(n_kv, n_tp, *args):
    (
        tokens,
        mix_gain,
        w_query,
        w_forget,
        w_input,
        w_outgate,
        lower_bound,
        state,
        head_gain,
        w_mixout,
        ffn_gain,
        w_gate,
        w_up,
        w_down,
    ) = args
    batch, cols = tokens.shape
    block, width = w_query.shape
    rows = state.shape[0]
    hidden = w_gate.shape[1]
    any_spec = pl.BlockSpec(memory_space=pl.ANY)
    vmem = pl.BlockSpec(memory_space=pltpu.VMEM)
    sems = [pltpu.SemaphoreType.DMA((16,))]
    for n in (n_tp, n_kv, n_kv, n_tp, n_kv, n_kv, n_tp):
        sems += [pltpu.SemaphoreType.DMA((max(n - 1, 1),))] * 2
    return pl.pallas_call(
        functools.partial(kernel, n_kv, n_tp),
        out_shape=(
            jax.ShapeDtypeStruct(tokens.shape, BF16),
            jax.ShapeDtypeStruct(state.shape, F32),
        ),
        in_specs=[
            any_spec,
            vmem,
            any_spec,
            any_spec,
            any_spec,
            any_spec,
            vmem,
            any_spec,
            vmem,
            any_spec,
            vmem,
            any_spec,
            any_spec,
            any_spec,
        ],
        out_specs=(vmem, any_spec),
        scratch_shapes=[
            pltpu.VMEM((4, block, width), BF16),
            pltpu.VMEM(state.shape, F32),
            pltpu.VMEM(w_mixout.shape, BF16),
            pltpu.VMEM(w_gate.shape, BF16),
            pltpu.VMEM(w_up.shape, BF16),
            pltpu.VMEM(w_down.shape, BF16),
            pltpu.VMEM(state.shape, F32),
            pltpu.VMEM((n_tp, batch, cols), BF16),
            pltpu.VMEM((batch, 4 * width + LANES), F32),
            pltpu.VMEM((n_kv, rows, 4 * width + LANES), BF16),
            pltpu.VMEM((n_kv, rows, 4 * width + LANES), BF16),
            pltpu.VMEM((n_kv, rows, width), BF16),
            pltpu.VMEM((batch, width), F32),
            pltpu.VMEM((n_tp, batch, block), BF16),
            pltpu.VMEM((n_tp, batch, cols), F32),
            pltpu.VMEM((batch, 2 * hidden + LANES), F32),
            pltpu.VMEM((n_kv, rows, 2 * hidden + LANES), BF16),
            pltpu.VMEM((n_kv, rows, 2 * hidden + LANES), BF16),
            pltpu.VMEM((n_kv, rows, hidden), BF16),
            pltpu.VMEM((batch, hidden), F32),
            pltpu.VMEM((n_tp, batch, cols), BF16),
            pltpu.VMEM((n_tp, batch, cols), BF16),
            *sems,
        ],
        compiler_params=pltpu.CompilerParams(collective_id=0, has_side_effects=True),
    )(
        tokens,
        mix_gain.reshape(1, -1),
        w_query,
        w_forget,
        w_input,
        w_outgate,
        lower_bound.reshape(1, -1),
        state,
        head_gain.reshape(1, -1),
        w_mixout,
        ffn_gain.reshape(1, -1),
        w_gate,
        w_up,
        w_down,
    )


def solution(mesh):
    return jax.shard_map(
        functools.partial(body, mesh.shape["kv"], mesh.shape["tp"]),
        mesh=mesh,
        in_specs=(
            P("grp", ("kv", "tp")),
            P("kv"),
            P("kv", "tp"),
            P("kv", "tp"),
            P("kv", "tp"),
            P("kv", "tp"),
            P("tp"),
            P(("grp", "kv"), "tp", None, None),
            P(),
            P("tp", "kv"),
            P("kv"),
            P("kv", "tp"),
            P("kv", "tp"),
            P("tp", "kv"),
        ),
        out_specs=(P("grp", ("kv", "tp")), P(("grp", "kv"), "tp", None, None)),
        check_vma=False,
    )
```

```python
import functools

import jax
import jax.numpy as jnp
from jax import lax
from jax.experimental import pallas as pl
from jax.experimental.pallas import tpu as pltpu
from jax.sharding import PartitionSpec as P

eps = 0.1
LANES = 128
CHUNKS = 4
F32 = jnp.float32
BF16 = jnp.bfloat16


def split_squares(squares):
    wide = jnp.broadcast_to(squares, (squares.shape[0], LANES))
    high = wide.astype(BF16).astype(F32)
    lane = lax.broadcasted_iota(jnp.int32, wide.shape, 1)
    return jnp.where(lane < LANES // 2, high, wide - high)


def join_squares(tile):
    return tile[:, :1] + tile[:, LANES // 2 : LANES // 2 + 1]


def row_of(ref):
    wide = ref[...].astype(F32)
    return jnp.concatenate([wide[i : i + 1] for i in range(wide.shape[0])], axis=1)


def tail(mixed_in, state_in, mixed, state, mixed_v, state_v, in_sem, out_sem):
    moves = [(mixed_in, mixed_v, mixed)]
    for i in range(state_v.shape[0]):
        moves.append((state_in.at[i], state_v.at[i], state.at[i]))
    first = [
        pltpu.make_async_copy(src, mid, in_sem.at[i]) for i, (src, mid, _) in enumerate(moves)
    ]
    second = [
        pltpu.make_async_copy(mid, dst, out_sem.at[i]) for i, (_, mid, dst) in enumerate(moves)
    ]
    for copy in first:
        copy.start()
    for one, two in zip(first, second):
        one.wait()
        two.start()
    for copy in second:
        copy.wait()


def kernel(
    n_kv,
    n_tp,
    chunks,
    tokens,
    mix_gain,
    w_query,
    w_forget,
    w_input,
    w_outgate,
    lower_bound,
    state,
    head_gain,
    w_mixout,
    ffn_gain,
    w_gate,
    w_up,
    w_down,
    mixed,
    new_state,
    proj_v,
    state_v,
    mixout_v,
    gate_v,
    up_v,
    down_v,
    next_v,
    mix_gain_v,
    bound_v,
    head_gain_v,
    ffn_gain_v,
    mixed_v,
    tok_buf,
    read_buf,
    read_f,
    mix_buf,
    resid_buf,
    down_send,
    down_recv,
    load_sem,
    store_sem,
    tok_s,
    tok_r,
    proj_s,
    proj_r,
    read_s,
    read_r,
    mix_s,
    mix_r,
    ffn_s,
    ffn_r,
    hid_s,
    hid_r,
    down_s,
    down_r,
    *chunk_bufs,
):
    kv = lax.axis_index("kv")
    tp = lax.axis_index("tp")
    rows, heads, size, _ = state.shape
    width = w_query.shape[1]
    hidden = w_gate.shape[1]
    cols = tokens.shape[1]
    model = w_query.shape[0] * n_kv
    proj_f, proj_send, proj_recv = (chunk_bufs[i : 12 : 3] for i in range(3))
    ffn_f, ffn_send, ffn_recv, hid_buf, hid_f = (chunk_bufs[12 + i :: 5] for i in range(5))

    loads = [
        pltpu.make_async_copy(src, dst, load_sem.at[i])
        for i, (src, dst) in enumerate(
            [
                (tokens, tok_buf.at[tp]),
                (mix_gain, mix_gain_v),
                (w_query, proj_v.at[0]),
                (w_forget, proj_v.at[1]),
                (w_input, proj_v.at[2]),
                (w_outgate, proj_v.at[3]),
                (lower_bound, bound_v),
                (head_gain, head_gain_v),
                (ffn_gain, ffn_gain_v),
                (state, state_v),
                (w_mixout, mixout_v),
                (w_gate, gate_v),
                (w_up, up_v),
                (w_down, down_v),
            ]
        )
    ]
    for load in loads:
        load.start()

    barrier = pltpu.get_barrier_semaphore()
    for d in range(1, n_tp):
        pl.semaphore_signal(barrier, inc=1, device_id={"tp": lax.rem(tp + d, n_tp)})
    for d in range(1, n_kv):
        pl.semaphore_signal(barrier, inc=1, device_id={"kv": lax.rem(kv + d, n_kv)})
    pl.semaphore_wait(barrier, n_tp - 1 + n_kv - 1)

    sent = []

    def exchange(axis, me, n, source, target, send_sem, recv_sem, base=0):
        copies = []
        for d in reversed(range(1, n)):
            peer = lax.rem(me + d, n)
            copy = pltpu.make_async_remote_copy(
                src_ref=source(peer),
                dst_ref=target(d),
                send_sem=send_sem.at[base + d - 1],
                recv_sem=recv_sem.at[base + d - 1],
                device_id={axis: peer},
            )
            copy.start()
            copies.append(copy)
        sent.extend(copies)
        return copies

    loads[0].wait()
    own = tok_buf.at[tp]
    for copy in exchange("tp", tp, n_tp, lambda p: own, lambda d: own, tok_s, tok_r):
        copy.wait_recv()
    loads[1].wait()
    block = jnp.concatenate([tok_buf[i].astype(F32) for i in range(n_tp)], axis=1)
    normed = (block * row_of(mix_gain_v)).astype(BF16)
    proj_f[0][:, width:] = split_squares(jnp.sum(block * block, axis=1, keepdims=True))

    proj_copies = []
    for i in range(4):
        loads[2 + i].wait()
        proj_f[i][:, :width] = jnp.dot(normed, proj_v[i], preferred_element_type=F32)
        send, recv = proj_send[i], proj_recv[i]
        for j in range(n_kv):
            send[j] = proj_f[i][j * rows : (j + 1) * rows, :].astype(BF16)
        proj_copies.append(
            exchange(
                "kv",
                kv,
                n_kv,
                lambda p: send.at[p],
                lambda d: recv.at[d - 1],
                proj_s,
                proj_r,
                i * (n_kv - 1),
            )
        )

    def collect(copies, send, recv):
        total = send[kv].astype(F32)
        for d, copy in zip(reversed(range(1, n_kv)), copies):
            copy.wait_recv()
            total += recv[d - 1].astype(F32)
        return total

    for load in loads[6:10]:
        load.wait()
    totals = [collect(*one) for one in zip(proj_copies, proj_send, proj_recv)]
    inv_rms = lax.rsqrt(join_squares(totals[0][:, width:]) / model + eps)
    query_raw, forget_raw, input_raw, gate_raw = (
        totals[i][:, :width] * inv_rms for i in range(4)
    )
    bounds = row_of(bound_v)
    forget = bounds + (1.0 - bounds) * jax.nn.sigmoid(forget_raw)
    key_in = (1.0 - bounds) * jax.nn.sigmoid(-forget_raw)
    query_act = query_raw * jax.nn.sigmoid(query_raw)
    gate_act = gate_raw * jax.nn.sigmoid(gate_raw)
    gain = row_of(head_gain_v)
    pad = jnp.zeros((-(3 * rows) % 8, width), F32)
    turned = jnp.concatenate([forget, key_in, query_act, pad], axis=0).T
    pieces = []
    for h in range(heads):
        here = slice(h * size, (h + 1) * size)
        readouts = []
        for b in range(rows):
            forget_c = turned[here, b : b + 1]
            key_c = turned[here, rows + b : rows + b + 1]
            query_c = turned[here, 2 * rows + b : 2 * rows + b + 1]
            after = forget_c * state_v[b, h] + key_c * input_raw[b : b + 1, here]
            next_v[b, h] = after
            readouts.append(jnp.sum(query_c * after, axis=0, keepdims=True))
        readout = jnp.concatenate(readouts, axis=0)
        head_rms = lax.rsqrt(jnp.mean(readout * readout, axis=1, keepdims=True) + eps)
        pieces.append(readout * head_rms * gain * gate_act[:, here])
    read_buf[kv] = jnp.concatenate(pieces, axis=1).astype(BF16)
    own_read = read_buf.at[kv]
    copies = exchange("kv", kv, n_kv, lambda p: own_read, lambda d: own_read, read_s, read_r)
    store = pltpu.make_async_copy(next_v, new_state, store_sem.at[0])
    store.start()
    loads[10].wait()
    for copy in copies:
        copy.wait_recv()
    for j in range(n_kv):
        read_f[j * rows : (j + 1) * rows, :] = read_buf[j].astype(F32)

    mix_buf[tp] = jnp.dot(
        read_f[...].astype(BF16), mixout_v[...], preferred_element_type=F32
    ).astype(BF16)
    own_mix = mix_buf.at[tp]
    copies = exchange("tp", tp, n_tp, lambda p: own_mix, lambda d: own_mix, mix_s, mix_r)
    for copy in copies:
        copy.wait_recv()
    mix_sum = mix_buf[0].astype(F32)
    for i in range(1, n_tp):
        mix_sum += mix_buf[i].astype(F32)
    resid = (block + mix_sum).astype(BF16).astype(F32)
    for i in range(n_tp):
        resid_buf[i] = resid[:, i * cols : (i + 1) * cols]
    normed_ffn = (resid * row_of(ffn_gain_v)).astype(BF16)
    ffn_f[0][:, 2 * chunks[0][1] :] = split_squares(jnp.sum(resid * resid, axis=1, keepdims=True))

    loads[11].wait()
    loads[12].wait()
    ffn_copies = []
    for c, (start, count) in enumerate(chunks):
        for i, weight in enumerate((gate_v, up_v)):
            ffn_f[c][:, i * count : (i + 1) * count] = jnp.dot(
                normed_ffn, weight[:, start : start + count], preferred_element_type=F32
            )
        send, recv = ffn_send[c], ffn_recv[c]
        for j in range(n_kv):
            send[j] = ffn_f[c][j * rows : (j + 1) * rows, :].astype(BF16)
        ffn_copies.append(
            exchange(
                "kv",
                kv,
                n_kv,
                lambda p: send.at[p],
                lambda d: recv.at[d - 1],
                ffn_s,
                ffn_r,
                c * (n_kv - 1),
            )
        )
    hid_copies = []
    for c, (start, count) in enumerate(chunks):
        total = collect(ffn_copies[c], ffn_send[c], ffn_recv[c])
        if c == 0:
            inv_rms = lax.rsqrt(join_squares(total[:, 2 * count :]) / model + eps)
        gate_sum = total[:, :count] * inv_rms
        up_sum = total[:, count : 2 * count] * inv_rms
        hid_buf[c][kv] = (gate_sum * jax.nn.sigmoid(gate_sum) * up_sum).astype(BF16)
        own_hid = hid_buf[c].at[kv]
        hid_copies.append(
            exchange(
                "kv",
                kv,
                n_kv,
                lambda p: own_hid,
                lambda d: own_hid,
                hid_s,
                hid_r,
                c * (n_kv - 1),
            )
        )

    loads[13].wait()
    down = None
    for c, (start, count) in enumerate(chunks):
        for copy in hid_copies[c]:
            copy.wait_recv()
        for j in range(n_kv):
            hid_f[c][j * rows : (j + 1) * rows, :] = hid_buf[c][j].astype(F32)
        term = jnp.dot(
            hid_f[c][...].astype(BF16),
            down_v[start : start + count, :],
            preferred_element_type=F32,
        )
        down = term if down is None else down + term
    for i in range(n_tp):
        down_send[i] = down[:, i * cols : (i + 1) * cols].astype(BF16)
    copies = exchange(
        "tp", tp, n_tp, lambda p: down_send.at[p], lambda d: down_recv.at[d - 1], down_s, down_r
    )
    result = down_send[tp].astype(F32)
    for d, copy in zip(reversed(range(1, n_tp)), copies):
        copy.wait_recv()
        result += down_recv[d - 1].astype(F32)
    mixed_v[...] = (resid_buf[tp] + result).astype(BF16)
    last = pltpu.make_async_copy(mixed_v, mixed, store_sem.at[1])
    last.start()

    for copy in sent:
        copy.wait_send()
    store.wait()
    last.wait()


def body(n_kv, n_tp, *args):
    (
        tokens,
        mix_gain,
        w_query,
        w_forget,
        w_input,
        w_outgate,
        lower_bound,
        state,
        head_gain,
        w_mixout,
        ffn_gain,
        w_gate,
        w_up,
        w_down,
    ) = args
    batch, cols = tokens.shape
    block, width = w_query.shape
    rows = state.shape[0]
    hidden = w_gate.shape[1]
    unit = 2 * LANES if hidden % (2 * LANES) == 0 else LANES
    units = hidden // unit
    count = -(-units // min(CHUNKS, units))
    chunks = [
        (i * unit, min(count, units - i) * unit) for i in range(0, units, count)
    ]
    any_spec = pl.BlockSpec(memory_space=pl.ANY)
    sems = [pltpu.SemaphoreType.DMA((14,)), pltpu.SemaphoreType.DMA((2,))]
    for n in (
        n_tp - 1,
        4 * (n_kv - 1),
        n_kv - 1,
        n_tp - 1,
        len(chunks) * (n_kv - 1),
        len(chunks) * (n_kv - 1),
        n_tp - 1,
    ):
        sems += [pltpu.SemaphoreType.DMA((max(n, 1),))] * 2
    bufs = []
    for i in range(4):
        wide = width + (LANES if i == 0 else 0)
        bufs += [
            pltpu.VMEM((batch, wide), F32),
            pltpu.VMEM((n_kv, rows, wide), BF16),
            pltpu.VMEM((n_kv, rows, wide), BF16),
        ]
    for i, (_, count) in enumerate(chunks):
        wide = 2 * count + (LANES if i == 0 else 0)
        bufs += [
            pltpu.VMEM((batch, wide), F32),
            pltpu.VMEM((n_kv, rows, wide), BF16),
            pltpu.VMEM((n_kv, rows, wide), BF16),
            pltpu.VMEM((n_kv, rows, count), BF16),
            pltpu.VMEM((batch, count), F32),
        ]
    small = [x.reshape(-1, LANES) for x in (mix_gain, lower_bound, head_gain, ffn_gain)]
    out_shape = (
        jax.ShapeDtypeStruct(tokens.shape, BF16),
        jax.ShapeDtypeStruct(state.shape, F32),
    )
    results = pl.pallas_call(
        functools.partial(kernel, n_kv, n_tp, chunks),
        out_shape=out_shape,
        in_specs=[any_spec] * 14,
        out_specs=(any_spec, any_spec),
        scratch_shapes=[
            pltpu.VMEM((4, block, width), BF16),
            pltpu.VMEM(state.shape, F32),
            pltpu.VMEM(w_mixout.shape, BF16),
            pltpu.VMEM(w_gate.shape, BF16),
            pltpu.VMEM(w_up.shape, BF16),
            pltpu.VMEM(w_down.shape, BF16),
            pltpu.VMEM(state.shape, F32),
            *[pltpu.VMEM(x.shape, x.dtype) for x in small],
            pltpu.VMEM(tokens.shape, BF16),
            pltpu.VMEM((n_tp, batch, cols), BF16),
            pltpu.VMEM((n_kv, rows, width), BF16),
            pltpu.VMEM((batch, width), F32),
            pltpu.VMEM((n_tp, batch, block), BF16),
            pltpu.VMEM((n_tp, batch, cols), F32),
            pltpu.VMEM((n_tp, batch, cols), BF16),
            pltpu.VMEM((n_tp, batch, cols), BF16),
            *sems,
            *bufs,
        ],
        compiler_params=pltpu.CompilerParams(collective_id=0, has_side_effects=True),
    )(
        tokens,
        small[0],
        w_query,
        w_forget,
        w_input,
        w_outgate,
        small[1],
        state,
        small[2],
        w_mixout,
        small[3],
        w_gate,
        w_up,
        w_down,
    )
    return pl.pallas_call(
        tail,
        out_shape=out_shape,
        in_specs=[any_spec] * 2,
        out_specs=(any_spec, any_spec),
        scratch_shapes=[
            pltpu.VMEM(tokens.shape, BF16),
            pltpu.VMEM(state.shape, F32),
            pltpu.SemaphoreType.DMA((1 + rows,)),
            pltpu.SemaphoreType.DMA((1 + rows,)),
        ],
    )(*results)


def solution(mesh):
    return jax.shard_map(
        functools.partial(body, mesh.shape["kv"], mesh.shape["tp"]),
        mesh=mesh,
        in_specs=(
            P("grp", ("kv", "tp")),
            P("kv"),
            P("kv", "tp"),
            P("kv", "tp"),
            P("kv", "tp"),
            P("kv", "tp"),
            P("tp"),
            P(("grp", "kv"), "tp", None, None),
            P(),
            P("tp", "kv"),
            P("kv"),
            P("kv", "tp"),
            P("kv", "tp"),
            P("tp", "kv"),
        ),
        out_specs=(P("grp", ("kv", "tp")), P(("grp", "kv"), "tp", None, None)),
        check_vma=False,
    )
```

```python
import functools

import jax
import jax.numpy as jnp
from jax import lax
from jax.experimental import pallas as pl
from jax.experimental.pallas import tpu as pltpu
from jax.sharding import PartitionSpec as P

eps = 0.1
LANES = 128
CHUNKS = 4
F32 = jnp.float32
BF16 = jnp.bfloat16


def split_squares(squares):
    wide = jnp.broadcast_to(squares, (squares.shape[0], LANES))
    high = wide.astype(BF16).astype(F32)
    lane = lax.broadcasted_iota(jnp.int32, wide.shape, 1)
    return jnp.where(lane < LANES // 2, high, wide - high)


def join_squares(tile):
    return tile[:, :1] + tile[:, LANES // 2 : LANES // 2 + 1]


def row_of(ref):
    wide = ref[...].astype(F32)
    return jnp.concatenate([wide[i : i + 1] for i in range(wide.shape[0])], axis=1)


def tail(mixed_in, state_in, mixed, state, sem):
    moves = [
        pltpu.make_async_copy(mixed_in, mixed, sem.at[0]),
        pltpu.make_async_copy(state_in, state, sem.at[1]),
    ]
    for move in moves:
        move.start()
    for move in moves:
        move.wait()


def kernel(
    n_kv,
    n_tp,
    chunks,
    tokens,
    mix_gain,
    w_query,
    w_forget,
    w_input,
    w_outgate,
    lower_bound,
    state,
    head_gain,
    w_mixout,
    ffn_gain,
    w_gate,
    w_up,
    w_down,
    mixed,
    new_state,
    proj_v,
    state_v,
    mixout_v,
    gate_v,
    up_v,
    down_v,
    mix_gain_v,
    bound_v,
    head_gain_v,
    ffn_gain_v,
    tok_buf,
    read_buf,
    read_f,
    mix_buf,
    resid_buf,
    down_send,
    down_recv,
    load_sem,
    tok_s,
    tok_r,
    proj_s,
    proj_r,
    read_s,
    read_r,
    mix_s,
    mix_r,
    ffn_s,
    ffn_r,
    hid_s,
    hid_r,
    down_s,
    down_r,
    *chunk_bufs,
):
    kv = lax.axis_index("kv")
    tp = lax.axis_index("tp")
    rows, heads, size, _ = state.shape
    width = w_query.shape[1]
    hidden = w_gate.shape[1]
    cols = tokens.shape[1]
    model = w_query.shape[0] * n_kv
    proj_f, proj_send, proj_recv = (chunk_bufs[i : 12 : 3] for i in range(3))
    ffn_f, ffn_send, ffn_recv, hid_buf, hid_f = (chunk_bufs[12 + i :: 5] for i in range(5))

    loads = [
        pltpu.make_async_copy(src, dst, load_sem.at[i])
        for i, (src, dst) in enumerate(
            [
                (tokens, tok_buf.at[tp]),
                (mix_gain, mix_gain_v),
                (w_query, proj_v.at[0]),
                (w_forget, proj_v.at[1]),
                (w_input, proj_v.at[2]),
                (w_outgate, proj_v.at[3]),
                (lower_bound, bound_v),
                (head_gain, head_gain_v),
                (ffn_gain, ffn_gain_v),
                (state, state_v),
                (w_mixout, mixout_v),
                (w_gate, gate_v),
                (w_up, up_v),
                (w_down, down_v),
            ]
        )
    ]
    for load in loads:
        load.start()

    barrier = pltpu.get_barrier_semaphore()
    for d in range(1, n_tp):
        pl.semaphore_signal(barrier, inc=1, device_id={"tp": lax.rem(tp + d, n_tp)})
    for d in range(1, n_kv):
        pl.semaphore_signal(barrier, inc=1, device_id={"kv": lax.rem(kv + d, n_kv)})
    pl.semaphore_wait(barrier, n_tp - 1 + n_kv - 1)

    sent = []

    def exchange(axis, me, n, source, target, send_sem, recv_sem, base=0):
        copies = []
        for d in reversed(range(1, n)):
            peer = lax.rem(me + d, n)
            copy = pltpu.make_async_remote_copy(
                src_ref=source(peer),
                dst_ref=target(d),
                send_sem=send_sem.at[base + d - 1],
                recv_sem=recv_sem.at[base + d - 1],
                device_id={axis: peer},
            )
            copy.start()
            copies.append(copy)
        sent.extend(copies)
        return copies

    loads[0].wait()
    own = tok_buf.at[tp]
    for copy in exchange("tp", tp, n_tp, lambda p: own, lambda d: own, tok_s, tok_r):
        copy.wait_recv()
    loads[1].wait()
    block = jnp.concatenate([tok_buf[i].astype(F32) for i in range(n_tp)], axis=1)
    normed = (block * row_of(mix_gain_v)).astype(BF16)
    proj_f[0][:, width:] = split_squares(jnp.sum(block * block, axis=1, keepdims=True))

    proj_copies = []
    for i in range(4):
        loads[2 + i].wait()
        proj_f[i][:, :width] = jnp.dot(normed, proj_v[i], preferred_element_type=F32)
        send, recv = proj_send[i], proj_recv[i]
        for j in range(n_kv):
            send[j] = proj_f[i][j * rows : (j + 1) * rows, :].astype(BF16)
        proj_copies.append(
            exchange(
                "kv",
                kv,
                n_kv,
                lambda p: send.at[p],
                lambda d: recv.at[d - 1],
                proj_s,
                proj_r,
                i * (n_kv - 1),
            )
        )

    def collect(copies, send, recv):
        total = send[kv].astype(F32)
        for d, copy in zip(reversed(range(1, n_kv)), copies):
            copy.wait_recv()
            total += recv[d - 1].astype(F32)
        return total

    for load in loads[6:10]:
        load.wait()
    totals = [collect(*one) for one in zip(proj_copies, proj_send, proj_recv)]
    inv_rms = lax.rsqrt(join_squares(totals[0][:, width:]) / model + eps)
    query_raw, forget_raw, input_raw, gate_raw = (
        totals[i][:, :width] * inv_rms for i in range(4)
    )
    bounds = row_of(bound_v)
    forget = bounds + (1.0 - bounds) * jax.nn.sigmoid(forget_raw)
    key_in = (1.0 - bounds) * jax.nn.sigmoid(-forget_raw)
    query_act = query_raw * jax.nn.sigmoid(query_raw)
    gate_act = gate_raw * jax.nn.sigmoid(gate_raw)
    gain = row_of(head_gain_v)
    pad = jnp.zeros((-(3 * rows) % 8, width), F32)
    turned = jnp.concatenate([forget, key_in, query_act, pad], axis=0).T
    pieces = []
    for h in range(heads):
        here = slice(h * size, (h + 1) * size)
        readouts = []
        for b in range(rows):
            forget_c = turned[here, b : b + 1]
            key_c = turned[here, rows + b : rows + b + 1]
            query_c = turned[here, 2 * rows + b : 2 * rows + b + 1]
            after = forget_c * state_v[b, h] + key_c * input_raw[b : b + 1, here]
            new_state[b, h] = after
            readouts.append(jnp.sum(query_c * after, axis=0, keepdims=True))
        readout = jnp.concatenate(readouts, axis=0)
        head_rms = lax.rsqrt(jnp.mean(readout * readout, axis=1, keepdims=True) + eps)
        pieces.append(readout * head_rms * gain * gate_act[:, here])
    read_buf[kv] = jnp.concatenate(pieces, axis=1).astype(BF16)
    own_read = read_buf.at[kv]
    copies = exchange("kv", kv, n_kv, lambda p: own_read, lambda d: own_read, read_s, read_r)
    loads[10].wait()
    for copy in copies:
        copy.wait_recv()
    for j in range(n_kv):
        read_f[j * rows : (j + 1) * rows, :] = read_buf[j].astype(F32)

    mix_buf[tp] = jnp.dot(
        read_f[...].astype(BF16), mixout_v[...], preferred_element_type=F32
    ).astype(BF16)
    own_mix = mix_buf.at[tp]
    copies = exchange("tp", tp, n_tp, lambda p: own_mix, lambda d: own_mix, mix_s, mix_r)
    for copy in copies:
        copy.wait_recv()
    mix_sum = mix_buf[0].astype(F32)
    for i in range(1, n_tp):
        mix_sum += mix_buf[i].astype(F32)
    resid = (block + mix_sum).astype(BF16).astype(F32)
    for i in range(n_tp):
        resid_buf[i] = resid[:, i * cols : (i + 1) * cols]
    normed_ffn = (resid * row_of(ffn_gain_v)).astype(BF16)
    ffn_f[0][:, 2 * chunks[0][1] :] = split_squares(jnp.sum(resid * resid, axis=1, keepdims=True))

    loads[11].wait()
    loads[12].wait()
    ffn_copies = []
    for c, (start, count) in enumerate(chunks):
        for i, weight in enumerate((gate_v, up_v)):
            ffn_f[c][:, i * count : (i + 1) * count] = jnp.dot(
                normed_ffn, weight[:, start : start + count], preferred_element_type=F32
            )
        send, recv = ffn_send[c], ffn_recv[c]
        for j in range(n_kv):
            send[j] = ffn_f[c][j * rows : (j + 1) * rows, :].astype(BF16)
        ffn_copies.append(
            exchange(
                "kv",
                kv,
                n_kv,
                lambda p: send.at[p],
                lambda d: recv.at[d - 1],
                ffn_s,
                ffn_r,
                c * (n_kv - 1),
            )
        )
    hid_copies = []
    for c, (start, count) in enumerate(chunks):
        total = collect(ffn_copies[c], ffn_send[c], ffn_recv[c])
        if c == 0:
            inv_rms = lax.rsqrt(join_squares(total[:, 2 * count :]) / model + eps)
        gate_sum = total[:, :count] * inv_rms
        up_sum = total[:, count : 2 * count] * inv_rms
        hid_buf[c][kv] = (gate_sum * jax.nn.sigmoid(gate_sum) * up_sum).astype(BF16)
        own_hid = hid_buf[c].at[kv]
        hid_copies.append(
            exchange(
                "kv",
                kv,
                n_kv,
                lambda p: own_hid,
                lambda d: own_hid,
                hid_s,
                hid_r,
                c * (n_kv - 1),
            )
        )

    loads[13].wait()
    down = None
    for c, (start, count) in enumerate(chunks):
        for copy in hid_copies[c]:
            copy.wait_recv()
        for j in range(n_kv):
            hid_f[c][j * rows : (j + 1) * rows, :] = hid_buf[c][j].astype(F32)
        term = jnp.dot(
            hid_f[c][...].astype(BF16),
            down_v[start : start + count, :],
            preferred_element_type=F32,
        )
        down = term if down is None else down + term
    for i in range(n_tp):
        down_send[i] = down[:, i * cols : (i + 1) * cols].astype(BF16)
    copies = exchange(
        "tp", tp, n_tp, lambda p: down_send.at[p], lambda d: down_recv.at[d - 1], down_s, down_r
    )
    result = down_send[tp].astype(F32)
    for d, copy in zip(reversed(range(1, n_tp)), copies):
        copy.wait_recv()
        result += down_recv[d - 1].astype(F32)
    mixed[...] = (resid_buf[tp] + result).astype(BF16)

    for copy in sent:
        copy.wait_send()


def body(n_kv, n_tp, *args):
    (
        tokens,
        mix_gain,
        w_query,
        w_forget,
        w_input,
        w_outgate,
        lower_bound,
        state,
        head_gain,
        w_mixout,
        ffn_gain,
        w_gate,
        w_up,
        w_down,
    ) = args
    batch, cols = tokens.shape
    block, width = w_query.shape
    rows = state.shape[0]
    hidden = w_gate.shape[1]
    unit = 2 * LANES if hidden % (2 * LANES) == 0 else LANES
    units = hidden // unit
    count = -(-units // min(CHUNKS, units))
    chunks = [
        (i * unit, min(count, units - i) * unit) for i in range(0, units, count)
    ]
    any_spec = pl.BlockSpec(memory_space=pl.ANY)
    vmem = pl.BlockSpec(memory_space=pltpu.VMEM)
    sems = [pltpu.SemaphoreType.DMA((14,))]
    for n in (
        n_tp - 1,
        4 * (n_kv - 1),
        n_kv - 1,
        n_tp - 1,
        len(chunks) * (n_kv - 1),
        len(chunks) * (n_kv - 1),
        n_tp - 1,
    ):
        sems += [pltpu.SemaphoreType.DMA((max(n, 1),))] * 2
    bufs = []
    for i in range(4):
        wide = width + (LANES if i == 0 else 0)
        bufs += [
            pltpu.VMEM((batch, wide), F32),
            pltpu.VMEM((n_kv, rows, wide), BF16),
            pltpu.VMEM((n_kv, rows, wide), BF16),
        ]
    for i, (_, count) in enumerate(chunks):
        wide = 2 * count + (LANES if i == 0 else 0)
        bufs += [
            pltpu.VMEM((batch, wide), F32),
            pltpu.VMEM((n_kv, rows, wide), BF16),
            pltpu.VMEM((n_kv, rows, wide), BF16),
            pltpu.VMEM((n_kv, rows, count), BF16),
            pltpu.VMEM((batch, count), F32),
        ]
    small = [x.reshape(-1, LANES) for x in (mix_gain, lower_bound, head_gain, ffn_gain)]
    results = pl.pallas_call(
        functools.partial(kernel, n_kv, n_tp, chunks),
        out_shape=(pltpu.VMEM(tokens.shape, BF16), pltpu.VMEM(state.shape, F32)),
        in_specs=[any_spec] * 14,
        out_specs=(vmem, vmem),
        scratch_shapes=[
            pltpu.VMEM((4, block, width), BF16),
            pltpu.VMEM(state.shape, F32),
            pltpu.VMEM(w_mixout.shape, BF16),
            pltpu.VMEM(w_gate.shape, BF16),
            pltpu.VMEM(w_up.shape, BF16),
            pltpu.VMEM(w_down.shape, BF16),
            *[pltpu.VMEM(x.shape, x.dtype) for x in small],
            pltpu.VMEM((n_tp, batch, cols), BF16),
            pltpu.VMEM((n_kv, rows, width), BF16),
            pltpu.VMEM((batch, width), F32),
            pltpu.VMEM((n_tp, batch, block), BF16),
            pltpu.VMEM((n_tp, batch, cols), F32),
            pltpu.VMEM((n_tp, batch, cols), BF16),
            pltpu.VMEM((n_tp, batch, cols), BF16),
            *sems,
            *bufs,
        ],
        compiler_params=pltpu.CompilerParams(collective_id=0, has_side_effects=True),
    )(
        tokens,
        small[0],
        w_query,
        w_forget,
        w_input,
        w_outgate,
        small[1],
        state,
        small[2],
        w_mixout,
        small[3],
        w_gate,
        w_up,
        w_down,
    )
    return pl.pallas_call(
        tail,
        out_shape=(
            jax.ShapeDtypeStruct(tokens.shape, BF16),
            jax.ShapeDtypeStruct(state.shape, F32),
        ),
        in_specs=[vmem] * 2,
        out_specs=(any_spec, any_spec),
        scratch_shapes=[pltpu.SemaphoreType.DMA((2,))],
    )(*[pltpu.with_memory_space_constraint(x, pltpu.VMEM) for x in results])


def solution(mesh):
    return jax.shard_map(
        functools.partial(body, mesh.shape["kv"], mesh.shape["tp"]),
        mesh=mesh,
        in_specs=(
            P("grp", ("kv", "tp")),
            P("kv"),
            P("kv", "tp"),
            P("kv", "tp"),
            P("kv", "tp"),
            P("kv", "tp"),
            P("tp"),
            P(("grp", "kv"), "tp", None, None),
            P(),
            P("tp", "kv"),
            P("kv"),
            P("kv", "tp"),
            P("kv", "tp"),
            P("tp", "kv"),
        ),
        out_specs=(P("grp", ("kv", "tp")), P(("grp", "kv"), "tp", None, None)),
        check_vma=False,
    )
```
